256 devices in a mesh: ep: 128 (over z, y, x), tp: 2 (over core).
Axes of the slice: x: 4, y: 4, z: 8, core: 2. Of those that a mesh axis runs over, the one named last changes fastest.
Arguments:
- tokens: bfloat16 [65536, 2048], P(('ep', 'tp')), may hold values from -6 to 6
- norm_gain: float32 [2048], replicated, may hold values from 0.1 to 1.9
- expert_ids: int32 [65536, 2], P(('ep', 'tp')), may hold values from 0 to 127, all different within a row; in each aligned block of 256 rows (0 to 255, 256 to 511, ...) at most 6 rows name the same one
- route_weights: float32 [65536, 2], P(('ep', 'tp')), may hold values from 0.2 to 1.2
- expert_gate: bfloat16 [128, 2048, 512], P('ep', None, 'tp'), may hold values from -0.125 to 0.125
- expert_up: bfloat16 [128, 2048, 512], P('ep', None, 'tp'), may hold values from -0.125 to 0.125
- expert_down: bfloat16 [128, 512, 2048], P('ep', 'tp'), may hold values from -0.25 to 0.25
- shared_gate: bfloat16 [2048, 512], P(None, 'tp'), may hold values from -0.125 to 0.125
- shared_up: bfloat16 [2048, 512], P(None, 'tp'), may hold values from -0.125 to 0.125
- shared_down: bfloat16 [512, 2048], P('tp'), may hold values from -0.25 to 0.25
Outputs:
- mixed: bfloat16 [65536, 2048], P(('ep', 'tp'))
The draws below stay inside these ranges and needn't reach their ends.
Inputs may be any that keep to these rules, and one draw needn't show every extreme that they name: `expert_ids`: each token names 2 different experts. Among the tokens of one device (aligned blocks of 256 rows) no expert is named by more than 6 tokens, and in every block some expert is named by exactly 6.
All inputs are finite; a program needn't handle non-finite values.
Results may differ from the reference program's by a relative error of at most 0.0075.
Values may be sent and summed in bfloat16 or wider, within the bound.
No kernel may reach another device: no remote copies, remote signals or barrier semaphores. Data moves between devices by JAX's collectives and lax.ppermute only.
A program may use at most 64 MiB of HBM per device.

```python
import math
import jax
import jax.numpy as jnp
import numpy as np
from jax import lax

D = 2048
DE = 512
DS = 512
TOP_K = 2
TOK_DEV = 256
EXPERTS = 128
CAP = 6
TOKENS = 65536
N_EP = 128
N_TP = 2


def block_scale(key, shape, pieces, smallest, top_value):
    factor_of, own = 1.0, jax.random.fold_in(key, 6)
    for axis_at, blocks in pieces:
        draws = jnp.exp(jax.random.uniform(jax.random.fold_in(own, axis_at), (blocks,), jnp.float32, smallest / len(pieces), top_value / len(pieces)))
        factor_of = factor_of * jnp.repeat(draws, shape[axis_at] // blocks).reshape([-1 if axis == axis_at else 1 for axis in range(len(shape))])
    return factor_of


def assign_block(key, own, number, rows, amount, top, most, skew):
    order = jax.random.permutation(key, amount)
    heavy_load, ordinary = load_shares(amount, rows * top, most, skew, True), load_shares(amount, rows * top, most, skew, False)
    places = jnp.arange(amount)

    def named(lengths, offset_by):
        used = int((lengths > 0).sum())
        fixed = max(1, used // 4)
        moved = fixed + (places - fixed + offset_by * (used - fixed)) % max(1, amount - fixed)
        return jnp.zeros((amount,), jnp.int32).at[order[jnp.where(places < fixed, places, moved)]].set(jnp.asarray(lengths, jnp.int32))

    lengths = jnp.where(number % 4 == 0, named(heavy_load, number // 4), named(ordinary, number - number // 4 - 1))
    mixed = jax.random.permutation(jax.random.fold_in(own, 3), amount)
    giver, sink = mixed[0:amount // 2 * 2:2], mixed[1:amount // 2 * 2:2]
    slack = jnp.minimum(lengths[giver] - 1, most - lengths[sink]) // 2
    slack = jnp.where((giver == order[0]) | (sink == order[0]) | (lengths[sink] == 0), 0, jnp.maximum(slack, 0))
    moved = jax.random.randint(jax.random.fold_in(own, 4), (amount // 2,), 0, 1 << 20) % (slack + 1)
    lengths = lengths.at[giver].add(-moved).at[sink].add(moved)
    items = jnp.searchsorted(jnp.cumsum(lengths), jnp.arange(rows * top), side="right").astype(jnp.int32)
    grid = items.reshape(top, rows).T
    grid = grid[jax.random.permutation(jax.random.fold_in(own, 1), rows)]
    offset_by = jax.random.randint(jax.random.fold_in(own, 2), (rows, 1), 0, top)
    return jnp.take_along_axis(grid, (jnp.arange(top)[None, :] + offset_by) % top, axis=1)


def load_shares(number_of, total, limit, skew, full):
    portions = [(1 << 20) // math.isqrt(standing ** skew) + 1 for standing in range(1, number_of + 1)]
    largest = limit if full else min(limit, max(-(-total // number_of), total * portions[0] // sum(portions)))
    least = 1 if total - largest >= number_of - 1 else 0
    holding, spare = [largest] + [least] * (number_of - 1), total - largest - least * (number_of - 1)
    while spare > 0:
        movable = [i for i in range(1, number_of) if holding[i] < largest] or [i for i in range(1, number_of) if holding[i] < limit]
        mass, left = sum([portions[i] for i in movable]), spare
        for i in movable:
            addition = min(limit - holding[i], max(1, left * portions[i] // mass), spare)
            holding[i] = holding[i] + addition
            spare = spare - addition
    return np.array(holding)


def noise(own_key, extent, spread, reach, split=(), kind=jnp.bfloat16):
    gain = block_scale(own_key, extent, split, -0.22, 0.18) if split else 1.0
    array = jax.random.normal(own_key, extent, jnp.float32) * spread * gain
    return jnp.minimum(jnp.maximum(array, -reach), reach).astype(kind)


def setup_inputs(seed: int = 0) -> dict:
    key_of = jax.random.split(jax.random.key(seed), 11)
    tokens = noise(key_of[0], (TOKENS, D), 1.0, 6.0, ((0, 256),))
    norm_gain = jnp.clip(1.0 + 0.18 * jax.random.normal(key_of[1], (D,), jnp.float32), 0.1, 1.9)
    expert_ids_keys = jax.random.split(jax.random.fold_in(key_of[2], 1), TOKENS // TOK_DEV)
    expert_ids_turns = jax.random.permutation(jax.random.fold_in(key_of[2], 3), TOKENS // TOK_DEV)
    expert_ids = jax.vmap(lambda own, number: assign_block(jax.random.fold_in(key_of[2], 2), own, number, TOK_DEV, EXPERTS, TOP_K, CAP, 2))(expert_ids_keys, expert_ids_turns).reshape((TOKENS, TOP_K))
    route_weights = jnp.clip(0.2 + 1 * jax.random.uniform(key_of[3], (TOKENS, TOP_K), jnp.float32) ** block_scale(key_of[3], (TOKENS, TOP_K), ((0, 256),), -0.2, 0.2), 0.2, 1.2)
    expert_gate = noise(key_of[4], (EXPERTS, D, DE), D ** -0.5, 0.125, ((0, 128), (2, 2)))
    expert_up = noise(key_of[5], (EXPERTS, D, DE), D ** -0.5, 0.125, ((0, 128), (2, 2)))
    expert_down = noise(key_of[6], (EXPERTS, DE, D), DE ** -0.5, 0.25, ((0, 128), (1, 2)))
    shared_gate = noise(key_of[7], (D, DS), D ** -0.5, 0.125, ((1, 2),))
    shared_up = noise(key_of[8], (D, DS), D ** -0.5, 0.125, ((1, 2),))
    shared_down = noise(key_of[9], (DS, D), DS ** -0.5, 0.25, ((0, 2),))
    return {"tokens": tokens, "norm_gain": norm_gain, "expert_ids": expert_ids, "route_weights": route_weights, "expert_gate": expert_gate, "expert_up": expert_up, "expert_down": expert_down, "shared_gate": shared_gate, "shared_up": shared_up, "shared_down": shared_down}


epsilon = 1e-06

def normalize(tokens, norm_gain):
    values = tokens.astype(jnp.float32)
    factor = lax.rsqrt(lax.optimization_barrier(jnp.mean(values * values, axis=1, keepdims=True)) + epsilon)
    return (values * factor * norm_gain[None, :]).astype(jnp.bfloat16)

def halves(row_block, gate_w, up_w, down_w):
    half_width = gate_w.shape[1] // N_TP
    summed = jnp.zeros((row_block.shape[0], down_w.shape[1]), jnp.float32)
    for portion in range(N_TP):
        first = portion * half_width
        gate_value = jnp.dot(row_block, gate_w[:, first:first + half_width], preferred_element_type=jnp.float32)
        up_value = jnp.dot(row_block, up_w[:, first:first + half_width], preferred_element_type=jnp.float32)
        hidden = (jax.nn.silu(gate_value) * up_value).astype(jnp.bfloat16)
        partial_value = jnp.dot(hidden, down_w[first:first + half_width], preferred_element_type=jnp.float32)
        rounded = lax.optimization_barrier(partial_value.astype(jnp.bfloat16))
        summed = summed + rounded.astype(jnp.float32)
    return summed

def reference(tokens, norm_gain, expert_ids, route_weights, expert_gate, expert_up, expert_down, shared_gate, shared_up, shared_down):
    normed = normalize(tokens, norm_gain)
    total_rows = tokens.shape[0]
    shared_out = halves(normed, shared_gate, shared_up, shared_down)
    flat_ids = expert_ids.reshape(-1).astype(jnp.int32)
    assigned = flat_ids.shape[0]
    ordering = jnp.argsort(flat_ids, stable=True).astype(jnp.int32)
    counts = jnp.bincount(flat_ids, length=EXPERTS).astype(jnp.int32)
    starts = (jnp.cumsum(counts) - counts).astype(jnp.int32)
    most_rows = N_EP * N_TP * CAP
    padded = jnp.concatenate([normed, jnp.zeros((1, D), jnp.bfloat16)], axis=0)
    flat_weights = route_weights.reshape(-1)

    def per_expert(totals, expert):
        slot_range = jnp.arange(most_rows, dtype=jnp.int32)
        filled = slot_range < counts[expert]
        row_index = jnp.minimum(starts[expert] + slot_range, assigned - 1)
        assign = jnp.where(filled, ordering[row_index], assigned)
        token_index = (assign // TOP_K).astype(jnp.int32)
        row_block = padded[token_index]
        expert_out = halves(row_block, expert_gate[expert], expert_up[expert], expert_down[expert]).astype(jnp.bfloat16)
        weight_rows = jnp.where(filled, flat_weights[jnp.minimum(assign, assigned - 1)], jnp.float32(0.0))
        totals = totals.at[token_index].add(expert_out.astype(jnp.float32) * weight_rows[:, None])
        return (totals, None)
    totals, _ = lax.scan(per_expert, jnp.zeros((total_rows + 1, D), jnp.float32), jnp.arange(EXPERTS, dtype=jnp.int32))
    routed = totals[:total_rows]
    return (routed + shared_out).astype(jnp.bfloat16)
```

```python
import functools

import jax
import jax.numpy as jnp
from jax import lax
from jax.experimental import pallas as pl
from jax.experimental.pallas import tpu as pltpu
from jax.sharding import PartitionSpec as P

epsilon = 1e-06
LANES = 128


def pack_kernel(capacity, tokens_ref, gain_ref, ids_ref, normed_ref, out_ref, pos_ref, tiles, pos_smem, sem):
    rows, width = tokens_ref.shape
    per_row = width // LANES
    top_count = ids_ref.shape[0]
    experts = out_ref.shape[0] // per_row // capacity
    ids = ids_ref[...]
    expert_iota = lax.broadcasted_iota(jnp.int32, (experts, rows), 0)
    named = [jnp.where(expert_iota == ids[j : j + 1, :], 1.0, 0.0) for j in range(top_count)]
    total = sum(named[1:], named[0]).astype(jnp.bfloat16)
    earlier = jnp.where(
        lax.broadcasted_iota(jnp.int32, (rows, rows), 0) < lax.broadcasted_iota(jnp.int32, (rows, rows), 1), 1.0, 0.0
    ).astype(jnp.bfloat16)
    before = jnp.dot(total, earlier, preferred_element_type=jnp.float32)
    for j in range(top_count):
        slot = jnp.sum(before * named[j], axis=0, keepdims=True).astype(jnp.int32)
        pos_ref[j : j + 1, :] = ids[j : j + 1, :] * capacity + slot
    copy = pltpu.make_async_copy(pos_ref, pos_smem, sem)
    copy.start()
    gain = gain_ref[...]
    step = 16

    def norm_rows(i, carry):
        first = pl.multiple_of(i * step, step)
        values = tokens_ref[pl.ds(first, step), :].astype(jnp.float32)
        factor = lax.rsqrt(jnp.mean(values * values, axis=1, keepdims=True) + epsilon)
        normed = (values * factor * gain).astype(jnp.bfloat16)
        normed_ref[pl.ds(first, step), :] = normed
        wide = normed.astype(jnp.float32)
        for k in range(per_row):
            tiles[pl.ds(first * per_row + k, step, stride=per_row), :] = wide[:, k * LANES : (k + 1) * LANES]
        return carry

    lax.fori_loop(0, rows // step, norm_rows, 0)
    copy.wait()

    unroll = 8

    def place(i, carry):
        for u in range(unroll):
            row = i * unroll + u
            tile = tiles[pl.ds(pl.multiple_of(row * per_row, per_row), per_row), :].astype(jnp.bfloat16)
            for j in range(top_count):
                at = pl.multiple_of(pos_smem[j, row] * per_row, per_row)
                out_ref[pl.ds(at, per_row), :] = tile
        return carry

    lax.fori_loop(0, rows // unroll, place, 0)


def pack(tokens, norm_gain, ids, experts, capacity):
    rows, width = tokens.shape
    per_row = width // LANES
    top_count = ids.shape[0]
    vmem = pl.BlockSpec(memory_space=pltpu.VMEM)
    return pl.pallas_call(
        functools.partial(pack_kernel, capacity),
        out_shape=(
            jax.ShapeDtypeStruct((rows, width), jnp.bfloat16),
            jax.ShapeDtypeStruct((experts * capacity * per_row, LANES), jnp.bfloat16),
            jax.ShapeDtypeStruct((top_count, rows), jnp.int32),
        ),
        in_specs=[vmem] * 3,
        out_specs=(vmem,) * 3,
        scratch_shapes=[
            pltpu.VMEM((rows * per_row, LANES), jnp.float32),
            pltpu.SMEM((top_count, rows), jnp.int32),
            pltpu.SemaphoreType.DMA,
        ],
        cost_estimate=pl.CostEstimate(flops=2 * experts * rows * rows, bytes_accessed=6 << 20, transcendentals=rows),
        name="pack_rows",
    )(tokens, norm_gain.reshape(1, width), ids)


def gated_sum(rows, gates, ups, downs):
    total = None
    for gate, up, down in zip(gates, ups, downs):
        gate_value = jnp.dot(rows, gate[...], preferred_element_type=jnp.float32)
        up_value = jnp.dot(rows, up[...], preferred_element_type=jnp.float32)
        hidden = (gate_value / (1.0 + jnp.exp(-gate_value)) * up_value).astype(jnp.bfloat16)
        part = jnp.dot(hidden, down[...], preferred_element_type=jnp.float32)
        part = part.astype(jnp.bfloat16).astype(jnp.float32)
        total = part if total is None else total + part
    return total


def expert_kernel(rows_ref, g0, u0, d0, g1, u1, d1, out_ref, tiles, rows):
    block, width = rows.shape
    per_row = width // LANES
    tiles[...] = rows_ref[...].astype(jnp.float32)
    for k in range(per_row):
        rows[:, k * LANES : (k + 1) * LANES] = tiles[pl.ds(k, block, stride=per_row), :].astype(jnp.bfloat16)
    total = gated_sum(rows[...], (g0, g1), (u0, u1), (d0, d1))
    for k in range(per_row):
        tiles[pl.ds(k, block, stride=per_row), :] = total[:, k * LANES : (k + 1) * LANES]
    out_ref[...] = tiles[...].astype(jnp.bfloat16)


def shared_kernel(rows_ref, g0, u0, d0, g1, u1, d1, out_ref):
    out_ref[...] = gated_sum(rows_ref[...], (g0, g1), (u0, u1), (d0, d1))


def weight_specs(weights):
    return [pl.BlockSpec(w.shape, lambda i: (0, 0)) for w in weights]


def ffn_cost(rows, weights):
    flops = 2 * rows * sum(w.shape[0] * w.shape[1] for w in weights)
    return pl.CostEstimate(flops=flops, bytes_accessed=12 << 20, transcendentals=rows * 512)


def expert_ffn(received, weights, block=128):
    width = weights[0].shape[0]
    per_row = width // LANES
    rows = received.shape[0] // per_row
    spec = pl.BlockSpec((block * per_row, LANES), lambda i: (i, 0))
    return pl.pallas_call(
        expert_kernel,
        grid=(rows // block,),
        out_shape=jax.ShapeDtypeStruct(received.shape, jnp.bfloat16),
        in_specs=[spec] + weight_specs(weights),
        out_specs=spec,
        scratch_shapes=[
            pltpu.VMEM((block * per_row, LANES), jnp.float32),
            pltpu.VMEM((block, width), jnp.bfloat16),
        ],
        cost_estimate=ffn_cost(rows, weights),
        name="expert_ffn",
    )(received, *weights)


def shared_ffn(normed, weights, block=128):
    rows, width = normed.shape
    spec = pl.BlockSpec((block, width), lambda i: (i, 0))
    return pl.pallas_call(
        shared_kernel,
        grid=(rows // block,),
        out_shape=jax.ShapeDtypeStruct((rows, width), jnp.float32),
        in_specs=[spec] + weight_specs(weights),
        out_specs=spec,
        cost_estimate=ffn_cost(rows, weights),
        name="shared_ffn",
    )(normed, *weights)


def combine_kernel(pos_ref, weight_ref, returned_ref, shared_ref, out_ref, tiles):
    rows, width = out_ref.shape
    per_row = width // LANES
    top_count = pos_ref.shape[0]
    unroll = 8

    def mix(i, carry):
        for u in range(unroll):
            row = i * unroll + u
            total = None
            for j in range(top_count):
                at = pl.multiple_of(pos_ref[j, row] * per_row, per_row)
                term = returned_ref[pl.ds(at, per_row), :].astype(jnp.float32) * weight_ref[j, row]
                total = term if total is None else total + term
            tiles[pl.ds(pl.multiple_of(row * per_row, per_row), per_row), :] = total
        return carry

    lax.fori_loop(0, rows // unroll, mix, 0)
    step = 16

    def finish(i, carry):
        first = pl.multiple_of(i * step, step)
        for k in range(per_row):
            cols = slice(k * LANES, (k + 1) * LANES)
            routed = tiles[pl.ds(first * per_row + k, step, stride=per_row), :]
            out_ref[pl.ds(first, step), cols] = (routed + shared_ref[pl.ds(first, step), cols]).astype(jnp.bfloat16)
        return carry

    lax.fori_loop(0, rows // step, finish, 0)


def combine(pos, route_weights, returned, shared_out):
    rows, width = shared_out.shape
    per_row = width // LANES
    vmem = pl.BlockSpec(memory_space=pltpu.VMEM)
    smem = pl.BlockSpec(memory_space=pltpu.SMEM)
    return pl.pallas_call(
        combine_kernel,
        out_shape=jax.ShapeDtypeStruct((rows, width), jnp.bfloat16),
        in_specs=[smem, smem, vmem, vmem],
        out_specs=vmem,
        scratch_shapes=[pltpu.VMEM((rows * per_row, LANES), jnp.float32)],
        cost_estimate=pl.CostEstimate(flops=4 * rows * width, bytes_accessed=6 << 20, transcendentals=0),
        name="combine_rows",
    )(pos, route_weights, returned, shared_out)


def swapped(own):
    pairs = [(i, lax.axis_size("tp") - 1 - i) for i in range(lax.axis_size("tp"))]
    return [lax.ppermute(w, "tp", pairs) for w in own]


def body(
    tokens,
    norm_gain,
    expert_ids,
    route_weights,
    expert_gate,
    expert_up,
    expert_down,
    shared_gate,
    shared_up,
    shared_down,
):
    tok_rows, width = tokens.shape
    top_count = expert_ids.shape[1]
    ep_size = lax.axis_size("ep")
    experts = expert_gate.shape[0] * ep_size
    capacity = 3 * tok_rows * top_count // (2 * experts)
    per_row = width // LANES
    normed, outgoing, pos = pack(tokens, norm_gain, expert_ids.T, experts, capacity)

    def exchange(rows):
        split = rows.reshape(ep_size, capacity * per_row, LANES)
        moved = lax.all_to_all(split, "ep", split_axis=0, concat_axis=0, tiled=True)
        return moved.reshape(rows.shape)

    received = exchange(outgoing)
    expert_own = [expert_gate[0], expert_up[0], expert_down[0]]
    shared_own = [shared_gate, shared_up, shared_down]
    shared_out = shared_ffn(normed, shared_own + swapped(shared_own))
    results = expert_ffn(received, expert_own + swapped(expert_own))
    returned = exchange(results)
    return combine(pos, route_weights.T, returned, shared_out)


def solution(mesh):
    placed = (
        P(("ep", "tp"), None),
        P(),
        P(("ep", "tp"), None),
        P(("ep", "tp"), None),
        P("ep", None, "tp"),
        P("ep", None, "tp"),
        P("ep", "tp", None),
        P(None, "tp"),
        P(None, "tp"),
        P("tp", None),
    )
    return jax.shard_map(
        body, mesh=mesh, in_specs=placed, out_specs=P(("ep", "tp"), None), check_vma=False
    )
```

```python
import functools

import jax
import jax.numpy as jnp
from jax import lax
from jax.experimental import pallas as pl
from jax.experimental.pallas import tpu as pltpu
from jax.sharding import PartitionSpec as P

epsilon = 1e-06
LANES = 128
STAGGER_NS = 32000


VMEM = pl.BlockSpec(memory_space=pltpu.VMEM)
SMEM = pl.BlockSpec(memory_space=pltpu.SMEM)
HBM = pl.BlockSpec(memory_space=pltpu.HBM)


def in_vmem(arrays):
    return [pltpu.with_memory_space_constraint(a, pltpu.VMEM) for a in arrays]


def in_hbm(arrays):
    return [pltpu.with_memory_space_constraint(a, pltpu.HBM) for a in arrays]


def pack_kernel(
    capacity, tokens_hbm, gain_ref, ids_ref, normed_hbm, out_hbm, pos_ref, tokens, normed, packed, tiles, pos_smem, sems
):
    rows, width = tokens.shape
    per_row = width // LANES
    top_count = ids_ref.shape[0]
    experts = packed.shape[0] // per_row // capacity
    load = pltpu.make_async_copy(tokens_hbm, tokens, sems.at[0])
    load.start()
    ids = ids_ref[...]
    expert_iota = lax.broadcasted_iota(jnp.int32, (experts, rows), 0)
    named = [jnp.where(expert_iota == ids[j : j + 1, :], 1.0, 0.0) for j in range(top_count)]
    total = sum(named[1:], named[0]).astype(jnp.bfloat16)
    earlier = jnp.where(
        lax.broadcasted_iota(jnp.int32, (rows, rows), 0) < lax.broadcasted_iota(jnp.int32, (rows, rows), 1), 1.0, 0.0
    ).astype(jnp.bfloat16)
    before = jnp.dot(total, earlier, preferred_element_type=jnp.float32)
    for j in range(top_count):
        slot = jnp.sum(before * named[j], axis=0, keepdims=True).astype(jnp.int32)
        pos_ref[j : j + 1, :] = ids[j : j + 1, :] * capacity + slot
    scalars = pltpu.make_async_copy(pos_ref, pos_smem, sems.at[1])
    scalars.start()
    gain = gain_ref[...]
    step = 16
    load.wait()

    def norm_rows(i, carry):
        first = pl.multiple_of(i * step, step)
        values = tokens[pl.ds(first, step), :].astype(jnp.float32)
        factor = lax.rsqrt(jnp.mean(values * values, axis=1, keepdims=True) + epsilon)
        rounded = (values * factor * gain).astype(jnp.bfloat16)
        normed[pl.ds(first, step), :] = rounded
        wide = rounded.astype(jnp.float32)
        for k in range(per_row):
            tiles[pl.ds(first * per_row + k, step, stride=per_row), :] = wide[:, k * LANES : (k + 1) * LANES]
        return carry

    lax.fori_loop(0, rows // step, norm_rows, 0)
    keep = pltpu.make_async_copy(normed, normed_hbm, sems.at[2])
    keep.start()
    scalars.wait()

    unroll = 16

    def place(i, carry):
        for u in range(unroll):
            row = i * unroll + u
            tile = tiles[pl.ds(pl.multiple_of(row * per_row, per_row), per_row), :].astype(jnp.bfloat16)
            for j in range(top_count):
                at = pl.multiple_of(pos_smem[j, row] * per_row, per_row)
                packed[pl.ds(at, per_row), :] = tile
        return carry

    lax.fori_loop(0, rows // unroll, place, 0)
    send = pltpu.make_async_copy(packed, out_hbm, sems.at[3])
    send.start()
    keep.wait()
    send.wait()
    if STAGGER_NS:

        @pl.when(lax.axis_index("tp") == 1)
        def _():
            pl.delay(STAGGER_NS)


def pack(tokens, norm_gain, ids, experts, capacity):
    rows, width = tokens.shape
    per_row = width // LANES
    top_count = ids.shape[0]
    slots = experts * capacity * per_row
    return pl.pallas_call(
        functools.partial(pack_kernel, capacity),
        out_shape=(
            pltpu.HBM((rows, width), jnp.bfloat16),
            pltpu.HBM((slots, LANES), jnp.bfloat16),
            jax.ShapeDtypeStruct((top_count, rows), jnp.int32),
        ),
        in_specs=[HBM, VMEM, VMEM],
        out_specs=(HBM, HBM, VMEM),
        scratch_shapes=[
            pltpu.VMEM((rows, width), jnp.bfloat16),
            pltpu.VMEM((rows, width), jnp.bfloat16),
            pltpu.VMEM((slots, LANES), jnp.bfloat16),
            pltpu.VMEM((rows * per_row, LANES), jnp.float32),
            pltpu.SMEM((top_count, rows), jnp.int32),
            pltpu.SemaphoreType.DMA((4,)),
        ],
        compiler_params=pltpu.CompilerParams(vmem_limit_bytes=20 << 20),
        cost_estimate=pl.CostEstimate(flops=2 * experts * rows * rows, bytes_accessed=6 << 20, transcendentals=rows),
        name="pack_rows",
    )(*in_hbm([tokens]), norm_gain.reshape(1, width), ids)


def gated_sum(rows, gates, ups, downs):
    total = None
    for gate, up, down in zip(gates, ups, downs):
        gate_value = jnp.dot(rows, gate[...], preferred_element_type=jnp.float32)
        up_value = jnp.dot(rows, up[...], preferred_element_type=jnp.float32)
        hidden = (gate_value / (1.0 + jnp.exp(-gate_value)) * up_value).astype(jnp.bfloat16)
        part = jnp.dot(hidden, down[...], preferred_element_type=jnp.float32)
        part = part.astype(jnp.bfloat16).astype(jnp.float32)
        total = part if total is None else total + part
    return total


def expert_kernel(blocks, rows_ref, *refs):
    weights_hbm, out_hbm, weights = refs[:6], refs[6], refs[7:13]
    tiles, rows, results, weight_sems, out_sems = refs[13:]
    total_rows, width = rows.shape
    per_row = width // LANES
    block = total_rows // blocks
    loads = [pltpu.make_async_copy(h, w, weight_sems.at[i]) for i, (h, w) in enumerate(zip(weights_hbm, weights))]
    for load in loads:
        load.start()

    def tile_range(i):
        return pl.ds(pl.multiple_of(i * block * per_row, block * per_row), block * per_row)

    def row_range(i):
        return pl.ds(pl.multiple_of(i * block, block), block)

    def untile(i, carry):
        tiles[...] = rows_ref[tile_range(i), :].astype(jnp.float32)
        for k in range(per_row):
            piece = tiles[pl.ds(k, block, stride=per_row), :]
            rows[row_range(i), k * LANES : (k + 1) * LANES] = piece.astype(jnp.bfloat16)
        return carry

    lax.fori_loop(0, blocks, untile, 0)
    for load in loads:
        load.wait()

    def store(i):
        return pltpu.make_async_copy(results.at[tile_range(i)], out_hbm.at[tile_range(i)], out_sems.at[i])

    def one_block(i, carry):
        total = gated_sum(rows[row_range(i), :], (weights[0], weights[3]), (weights[1], weights[4]), (weights[2], weights[5]))
        for k in range(per_row):
            tiles[pl.ds(k, block, stride=per_row), :] = total[:, k * LANES : (k + 1) * LANES]
        results[tile_range(i), :] = tiles[...].astype(jnp.bfloat16)
        store(i).start()
        return carry

    lax.fori_loop(0, blocks, one_block, 0)
    for i in range(blocks):
        store(i).wait()


def shared_kernel(rows_hbm, *refs):
    sources, out_hbm, held, out, sems = (rows_hbm, *refs[:6]), refs[6], refs[7:14], refs[14], refs[15]
    loads = [pltpu.make_async_copy(h, w, sems.at[i]) for i, (h, w) in enumerate(zip(sources, held))]
    for load in loads:
        load.start()
    for load in loads:
        load.wait()
    out[...] = gated_sum(held[0][...], (held[1], held[4]), (held[2], held[5]), (held[3], held[6]))
    store = pltpu.make_async_copy(out, out_hbm, sems.at[7])
    store.start()
    store.wait()


def ffn_cost(rows, weights):
    flops = 2 * rows * sum(w.shape[0] * w.shape[1] for w in weights)
    return pl.CostEstimate(flops=flops, bytes_accessed=12 << 20, transcendentals=rows * 512)


def expert_ffn(received, weights):
    width = weights[0].shape[0]
    per_row = width // LANES
    rows = received.shape[0] // per_row
    blocks = 2
    return pl.pallas_call(
        functools.partial(expert_kernel, blocks),
        out_shape=pltpu.HBM(received.shape, jnp.bfloat16),
        in_specs=[VMEM] + [HBM] * 6,
        out_specs=HBM,
        scratch_shapes=[pltpu.VMEM(w.shape, w.dtype) for w in weights]
        + [
            pltpu.VMEM((rows // blocks * per_row, LANES), jnp.float32),
            pltpu.VMEM((rows, width), jnp.bfloat16),
            pltpu.VMEM(received.shape, jnp.bfloat16),
            pltpu.SemaphoreType.DMA((6,)),
            pltpu.SemaphoreType.DMA((blocks,)),
        ],
        compiler_params=pltpu.CompilerParams(vmem_limit_bytes=40 << 20),
        cost_estimate=ffn_cost(rows, weights),
        name="expert_ffn",
    )(*in_vmem([received]), *in_hbm(weights))


def shared_ffn(normed, weights):
    rows, width = normed.shape
    return pl.pallas_call(
        shared_kernel,
        out_shape=pltpu.HBM((rows, width), jnp.float32),
        in_specs=[HBM] * 7,
        out_specs=HBM,
        scratch_shapes=[pltpu.VMEM(a.shape, a.dtype) for a in [normed] + weights]
        + [pltpu.VMEM((rows, width), jnp.float32), pltpu.SemaphoreType.DMA((8,))],
        compiler_params=pltpu.CompilerParams(vmem_limit_bytes=30 << 20),
        cost_estimate=ffn_cost(rows, weights),
        name="shared_ffn",
    )(*in_hbm([normed] + weights))


def combine_kernel(pos_ref, weight_ref, returned_ref, shared_hbm, out_hbm, shared, tiles, out, load_sem, out_sems):
    rows, width = out.shape
    per_row = width // LANES
    top_count = pos_ref.shape[0]
    load = pltpu.make_async_copy(shared_hbm, shared, load_sem)
    load.start()
    unroll = 16
    parts = out_sems.shape[0]
    part = rows // parts
    step = 16

    def mix(i, carry):
        for u in range(unroll):
            row = i * unroll + u
            total = None
            for j in range(top_count):
                at = pl.multiple_of(pos_ref[j, row] * per_row, per_row)
                term = returned_ref[pl.ds(at, per_row), :].astype(jnp.float32) * weight_ref[j, row]
                total = term if total is None else total + term
            tiles[pl.ds(pl.multiple_of(row * per_row, per_row), per_row), :] = total
        return carry

    def finish(i, carry):
        first = pl.multiple_of(i * step, step)
        for k in range(per_row):
            cols = slice(k * LANES, (k + 1) * LANES)
            routed = tiles[pl.ds(first * per_row + k, step, stride=per_row), :]
            out[pl.ds(first, step), cols] = (routed + shared[pl.ds(first, step), cols]).astype(jnp.bfloat16)
        return carry

    stores = []
    for p in range(parts):
        lax.fori_loop(p * part // unroll, (p + 1) * part // unroll, mix, 0)
        if p == 0:
            load.wait()
        lax.fori_loop(p * part // step, (p + 1) * part // step, finish, 0)
        at = pl.ds(p * part, part)
        stores.append(pltpu.make_async_copy(out.at[at], out_hbm.at[at], out_sems.at[p]))
        stores[-1].start()
    for store in stores:
        store.wait()


def combine(pos, route_weights, returned, shared_out):
    rows, width = shared_out.shape
    per_row = width // LANES
    return pl.pallas_call(
        combine_kernel,
        out_shape=pltpu.HBM((rows, width), jnp.bfloat16),
        in_specs=[SMEM, SMEM, VMEM, HBM],
        out_specs=HBM,
        scratch_shapes=[
            pltpu.VMEM((rows, width), jnp.float32),
            pltpu.VMEM((rows * per_row, LANES), jnp.float32),
            pltpu.VMEM((rows, width), jnp.bfloat16),
            pltpu.SemaphoreType.DMA,
            pltpu.SemaphoreType.DMA((2,)),
        ],
        compiler_params=pltpu.CompilerParams(vmem_limit_bytes=20 << 20),
        cost_estimate=pl.CostEstimate(flops=4 * rows * width, bytes_accessed=6 << 20, transcendentals=0),
        name="combine_rows",
    )(pos, route_weights, *in_vmem([returned]), *in_hbm([shared_out]))


def swapped(own):
    pairs = [(i, lax.axis_size("tp") - 1 - i) for i in range(lax.axis_size("tp"))]
    return [lax.ppermute(w, "tp", pairs) for w in own]


def body(
    tokens,
    norm_gain,
    expert_ids,
    route_weights,
    expert_gate,
    expert_up,
    expert_down,
    shared_gate,
    shared_up,
    shared_down,
):
    tok_rows, width = tokens.shape
    top_count = expert_ids.shape[1]
    ep_size = lax.axis_size("ep")
    experts = expert_gate.shape[0] * ep_size
    capacity = 3 * tok_rows * top_count // (2 * experts)
    per_row = width // LANES
    normed, outgoing, pos = pack(tokens, norm_gain, expert_ids.T, experts, capacity)

    def exchange(rows):
        split = rows.reshape(ep_size, capacity * per_row, LANES)
        moved = lax.all_to_all(split, "ep", split_axis=0, concat_axis=0, tiled=True)
        return moved.reshape(rows.shape)

    received = exchange(outgoing)
    expert_own = [expert_gate[0], expert_up[0], expert_down[0]]
    shared_own = [shared_gate, shared_up, shared_down]
    shared_out = shared_ffn(normed, shared_own + swapped(shared_own))
    results = expert_ffn(received, expert_own + swapped(expert_own))
    returned = exchange(results)
    return combine(pos, route_weights.T, returned, shared_out)


def solution(mesh):
    placed = (
        P(("ep", "tp"), None),
        P(),
        P(("ep", "tp"), None),
        P(("ep", "tp"), None),
        P("ep", None, "tp"),
        P("ep", None, "tp"),
        P("ep", "tp", None),
        P(None, "tp"),
        P(None, "tp"),
        P("tp", None),
    )
    return jax.shard_map(
        body, mesh=mesh, in_specs=placed, out_specs=P(("ep", "tp"), None), check_vma=False
    )
```

```python
import functools

import jax
import jax.numpy as jnp
from jax import lax
from jax.experimental import pallas as pl
from jax.experimental.pallas import tpu as pltpu
from jax.sharding import PartitionSpec as P

epsilon = 1e-06
LANES = 128
STAGGER_NS = 33000


VMEM = pl.BlockSpec(memory_space=pltpu.VMEM)
HBM = pl.BlockSpec(memory_space=pltpu.HBM)


def in_vmem(arrays):
    return [pltpu.with_memory_space_constraint(a, pltpu.VMEM) for a in arrays]


def in_hbm(arrays):
    return [pltpu.with_memory_space_constraint(a, pltpu.HBM) for a in arrays]


def pack_kernel(
    capacity,
    tokens_hbm,
    gain_hbm,
    ids_hbm,
    normed_hbm,
    out_hbm,
    pos_hbm,
    tokens,
    gain_ref,
    ids_ref,
    pos_ref,
    normed,
    packed,
    tiles,
    pos_smem,
    sems,
):
    rows, width = tokens.shape
    per_row = width // LANES
    top_count = ids_ref.shape[0]
    experts = packed.shape[0] // per_row // capacity
    ids_load = pltpu.make_async_copy(ids_hbm, ids_ref, sems.at[4])
    gain_load = pltpu.make_async_copy(gain_hbm, gain_ref, sems.at[5])
    load = pltpu.make_async_copy(tokens_hbm, tokens, sems.at[0])
    for copy in (ids_load, gain_load, load):
        copy.start()
    ids_load.wait()
    ids = ids_ref[...]
    expert_iota = lax.broadcasted_iota(jnp.int32, (experts, rows), 0)
    named = [jnp.where(expert_iota == ids[j : j + 1, :], 1.0, 0.0) for j in range(top_count)]
    total = sum(named[1:], named[0]).astype(jnp.bfloat16)
    earlier = jnp.where(
        lax.broadcasted_iota(jnp.int32, (rows, rows), 0) < lax.broadcasted_iota(jnp.int32, (rows, rows), 1), 1.0, 0.0
    ).astype(jnp.bfloat16)
    before = jnp.dot(total, earlier, preferred_element_type=jnp.float32)
    for j in range(top_count):
        slot = jnp.sum(before * named[j], axis=0, keepdims=True).astype(jnp.int32)
        pos_ref[j : j + 1, :] = ids[j : j + 1, :] * capacity + slot
    scalars = pltpu.make_async_copy(pos_ref, pos_smem, sems.at[1])
    scalars.start()
    pos_keep = pltpu.make_async_copy(pos_ref, pos_hbm, sems.at[6])
    pos_keep.start()
    gain_load.wait()
    gain = gain_ref[...]
    step = 16
    load.wait()

    def norm_rows(i, carry):
        first = pl.multiple_of(i * step, step)
        values = tokens[pl.ds(first, step), :].astype(jnp.float32)
        factor = lax.rsqrt(jnp.mean(values * values, axis=1, keepdims=True) + epsilon)
        rounded = (values * factor * gain).astype(jnp.bfloat16)
        normed[pl.ds(first, step), :] = rounded
        wide = rounded.astype(jnp.float32)
        for k in range(per_row):
            tiles[pl.ds(first * per_row + k, step, stride=per_row), :] = wide[:, k * LANES : (k + 1) * LANES]
        return carry

    lax.fori_loop(0, rows // step, norm_rows, 0, unroll=8)
    keep = pltpu.make_async_copy(normed, normed_hbm, sems.at[2])
    keep.start()
    scalars.wait()

    unroll = 16

    def place(i, carry):
        for u in range(unroll):
            row = i * unroll + u
            tile = tiles[pl.ds(pl.multiple_of(row * per_row, per_row), per_row), :].astype(jnp.bfloat16)
            for j in range(top_count):
                at = pl.multiple_of(pos_smem[j, row] * per_row, per_row)
                packed[pl.ds(at, per_row), :] = tile
        return carry

    lax.fori_loop(0, rows // unroll, place, 0)
    send = pltpu.make_async_copy(packed, out_hbm, sems.at[3])
    send.start()
    pos_keep.wait()
    keep.wait()
    send.wait()
    if STAGGER_NS:

        @pl.when(lax.axis_index("tp") == 1)
        def _():
            pl.delay(STAGGER_NS)


def pack(tokens, norm_gain, ids, experts, capacity):
    rows, width = tokens.shape
    per_row = width // LANES
    top_count = ids.shape[0]
    slots = experts * capacity * per_row
    return pl.pallas_call(
        functools.partial(pack_kernel, capacity),
        out_shape=(
            pltpu.HBM((rows, width), jnp.bfloat16),
            pltpu.HBM((slots, LANES), jnp.bfloat16),
            pltpu.HBM((top_count, rows), jnp.int32),
        ),
        in_specs=[HBM] * 3,
        out_specs=(HBM,) * 3,
        scratch_shapes=[
            pltpu.VMEM((rows, width), jnp.bfloat16),
            pltpu.VMEM((1, width), jnp.float32),
            pltpu.VMEM((top_count, rows), jnp.int32),
            pltpu.VMEM((top_count, rows), jnp.int32),
            pltpu.VMEM((rows, width), jnp.bfloat16),
            pltpu.VMEM((slots, LANES), jnp.bfloat16),
            pltpu.VMEM((rows * per_row, LANES), jnp.float32),
            pltpu.SMEM((top_count, rows), jnp.int32),
            pltpu.SemaphoreType.DMA((7,)),
        ],
        compiler_params=pltpu.CompilerParams(vmem_limit_bytes=20 << 20),
        cost_estimate=pl.CostEstimate(flops=2 * experts * rows * rows, bytes_accessed=6 << 20, transcendentals=rows),
        name="pack_rows",
    )(*in_hbm([tokens, norm_gain.reshape(1, width), ids]))


def gated_sum(rows, gates, ups, downs):
    total = None
    for gate, up, down in zip(gates, ups, downs):
        gate_value = jnp.dot(rows, gate[...], preferred_element_type=jnp.float32)
        up_value = jnp.dot(rows, up[...], preferred_element_type=jnp.float32)
        hidden = (gate_value / (1.0 + jnp.exp(-gate_value)) * up_value).astype(jnp.bfloat16)
        part = jnp.dot(hidden, down[...], preferred_element_type=jnp.float32)
        part = part.astype(jnp.bfloat16).astype(jnp.float32)
        total = part if total is None else total + part
    return total


def expert_kernel(blocks, rows_ref, *refs):
    weights_hbm, out_hbm, weights = refs[:6], refs[6], refs[7:13]
    tiles, rows, results, weight_sems, out_sems = refs[13:]
    total_rows, width = rows.shape
    per_row = width // LANES
    block = total_rows // blocks
    loads = [pltpu.make_async_copy(h, w, weight_sems.at[i]) for i, (h, w) in enumerate(zip(weights_hbm, weights))]
    for load in loads:
        load.start()

    def tile_range(i):
        return pl.ds(pl.multiple_of(i * block * per_row, block * per_row), block * per_row)

    def row_range(i):
        return pl.ds(pl.multiple_of(i * block, block), block)

    def untile(i, carry):
        tiles[...] = rows_ref[tile_range(i), :].astype(jnp.float32)
        for k in range(per_row):
            piece = tiles[pl.ds(k, block, stride=per_row), :]
            rows[row_range(i), k * LANES : (k + 1) * LANES] = piece.astype(jnp.bfloat16)
        return carry

    lax.fori_loop(0, blocks, untile, 0)
    for load in loads:
        load.wait()

    def store(i):
        return pltpu.make_async_copy(results.at[tile_range(i)], out_hbm.at[tile_range(i)], out_sems.at[i])

    def one_block(i, carry):
        total = gated_sum(rows[row_range(i), :], (weights[0], weights[3]), (weights[1], weights[4]), (weights[2], weights[5]))
        for k in range(per_row):
            tiles[pl.ds(k, block, stride=per_row), :] = total[:, k * LANES : (k + 1) * LANES]
        results[tile_range(i), :] = tiles[...].astype(jnp.bfloat16)
        store(i).start()
        return carry

    lax.fori_loop(0, blocks, one_block, 0)
    for i in range(blocks):
        store(i).wait()


def shared_kernel(rows_hbm, *refs):
    sources, out_hbm, held, out, sems = (rows_hbm, *refs[:6]), refs[6], refs[7:14], refs[14], refs[15]
    loads = [pltpu.make_async_copy(h, w, sems.at[i]) for i, (h, w) in enumerate(zip(sources, held))]
    for load in loads:
        load.start()
    for load in loads:
        load.wait()
    out[...] = gated_sum(held[0][...], (held[1], held[4]), (held[2], held[5]), (held[3], held[6]))
    store = pltpu.make_async_copy(out, out_hbm, sems.at[7])
    store.start()
    store.wait()


def ffn_cost(rows, weights):
    flops = 2 * rows * sum(w.shape[0] * w.shape[1] for w in weights)
    return pl.CostEstimate(flops=flops, bytes_accessed=12 << 20, transcendentals=rows * 512)


def expert_ffn(received, weights):
    width = weights[0].shape[0]
    per_row = width // LANES
    rows = received.shape[0] // per_row
    blocks = 2
    return pl.pallas_call(
        functools.partial(expert_kernel, blocks),
        out_shape=pltpu.HBM(received.shape, jnp.bfloat16),
        in_specs=[VMEM] + [HBM] * 6,
        out_specs=HBM,
        scratch_shapes=[pltpu.VMEM(w.shape, w.dtype) for w in weights]
        + [
            pltpu.VMEM((rows // blocks * per_row, LANES), jnp.float32),
            pltpu.VMEM((rows, width), jnp.bfloat16),
            pltpu.VMEM(received.shape, jnp.bfloat16),
            pltpu.SemaphoreType.DMA((6,)),
            pltpu.SemaphoreType.DMA((blocks,)),
        ],
        compiler_params=pltpu.CompilerParams(vmem_limit_bytes=40 << 20),
        cost_estimate=ffn_cost(rows, weights),
        name="expert_ffn",
    )(*in_vmem([received]), *in_hbm(weights))


def shared_ffn(normed, weights):
    rows, width = normed.shape
    return pl.pallas_call(
        shared_kernel,
        out_shape=pltpu.HBM((rows, width), jnp.float32),
        in_specs=[HBM] * 7,
        out_specs=HBM,
        scratch_shapes=[pltpu.VMEM(a.shape, a.dtype) for a in [normed] + weights]
        + [pltpu.VMEM((rows, width), jnp.float32), pltpu.SemaphoreType.DMA((8,))],
        compiler_params=pltpu.CompilerParams(vmem_limit_bytes=30 << 20),
        cost_estimate=ffn_cost(rows, weights),
        name="shared_ffn",
    )(*in_hbm([normed] + weights))


def combine_kernel(pos_hbm, weight_hbm, returned_ref, shared_hbm, out_hbm, pos_ref, weight_ref, shared, tiles, out, load_sems, out_sems):
    rows, width = out.shape
    per_row = width // LANES
    top_count = pos_ref.shape[0]
    scalars = [
        pltpu.make_async_copy(pos_hbm, pos_ref, load_sems.at[0]),
        pltpu.make_async_copy(weight_hbm, weight_ref, load_sems.at[1]),
    ]
    load = pltpu.make_async_copy(shared_hbm, shared, load_sems.at[2])
    for copy in scalars + [load]:
        copy.start()
    unroll = 16
    parts = out_sems.shape[0]
    part = rows // parts
    step = 16

    def mix(i, carry):
        for u in range(unroll):
            row = i * unroll + u
            total = None
            for j in range(top_count):
                at = pl.multiple_of(pos_ref[j, row] * per_row, per_row)
                term = returned_ref[pl.ds(at, per_row), :].astype(jnp.float32) * weight_ref[j, row]
                total = term if total is None else total + term
            tiles[pl.ds(pl.multiple_of(row * per_row, per_row), per_row), :] = total
        return carry

    def finish(i, carry):
        first = pl.multiple_of(i * step, step)
        for k in range(per_row):
            cols = slice(k * LANES, (k + 1) * LANES)
            routed = tiles[pl.ds(first * per_row + k, step, stride=per_row), :]
            out[pl.ds(first, step), cols] = (routed + shared[pl.ds(first, step), cols]).astype(jnp.bfloat16)
        return carry

    stores = []
    for copy in scalars:
        copy.wait()
    for p in range(parts):
        lax.fori_loop(p * part // unroll, (p + 1) * part // unroll, mix, 0)
        if p == 0:
            load.wait()
        lax.fori_loop(p * part // step, (p + 1) * part // step, finish, 0, unroll=2)
        at = pl.ds(p * part, part)
        stores.append(pltpu.make_async_copy(out.at[at], out_hbm.at[at], out_sems.at[p]))
        stores[-1].start()
    for store in stores:
        store.wait()


def combine(pos, route_weights, returned, shared_out):
    rows, width = shared_out.shape
    per_row = width // LANES
    return pl.pallas_call(
        combine_kernel,
        out_shape=pltpu.HBM((rows, width), jnp.bfloat16),
        in_specs=[HBM, HBM, VMEM, HBM],
        out_specs=HBM,
        scratch_shapes=[
            pltpu.SMEM(pos.shape, pos.dtype),
            pltpu.SMEM(route_weights.shape, route_weights.dtype),
            pltpu.VMEM((rows, width), jnp.float32),
            pltpu.VMEM((rows * per_row, LANES), jnp.float32),
            pltpu.VMEM((rows, width), jnp.bfloat16),
            pltpu.SemaphoreType.DMA((3,)),
            pltpu.SemaphoreType.DMA((2,)),
        ],
        compiler_params=pltpu.CompilerParams(vmem_limit_bytes=20 << 20),
        cost_estimate=pl.CostEstimate(flops=4 * rows * width, bytes_accessed=6 << 20, transcendentals=0),
        name="combine_rows",
    )(*in_hbm([pos, route_weights]), *in_vmem([returned]), *in_hbm([shared_out]))


def swapped(own):
    pairs = [(i, lax.axis_size("tp") - 1 - i) for i in range(lax.axis_size("tp"))]
    return [lax.ppermute(w, "tp", pairs) for w in own]


def body(
    tokens,
    norm_gain,
    expert_ids,
    route_weights,
    expert_gate,
    expert_up,
    expert_down,
    shared_gate,
    shared_up,
    shared_down,
):
    tok_rows, width = tokens.shape
    top_count = expert_ids.shape[1]
    ep_size = lax.axis_size("ep")
    experts = expert_gate.shape[0] * ep_size
    capacity = 3 * tok_rows * top_count // (2 * experts)
    per_row = width // LANES
    normed, outgoing, pos = pack(tokens, norm_gain, expert_ids.T, experts, capacity)

    def exchange(rows):
        split = rows.reshape(ep_size, capacity * per_row, LANES)
        moved = lax.all_to_all(split, "ep", split_axis=0, concat_axis=0, tiled=True)
        return moved.reshape(rows.shape)

    received = exchange(outgoing)
    expert_own = [expert_gate[0], expert_up[0], expert_down[0]]
    shared_own = [shared_gate, shared_up, shared_down]
    shared_out = shared_ffn(normed, shared_own + swapped(shared_own))
    results = expert_ffn(received, expert_own + swapped(expert_own))
    returned = exchange(results)
    return combine(pos, route_weights.T, returned, shared_out)


def solution(mesh):
    placed = (
        P(("ep", "tp"), None),
        P(),
        P(("ep", "tp"), None),
        P(("ep", "tp"), None),
        P("ep", None, "tp"),
        P("ep", None, "tp"),
        P("ep", "tp", None),
        P(None, "tp"),
        P(None, "tp"),
        P("tp", None),
    )
    return jax.shard_map(
        body, mesh=mesh, in_specs=placed, out_specs=P(("ep", "tp"), None), check_vma=False
    )
```

```python
import functools

import jax
import jax.numpy as jnp
from jax import lax
from jax.experimental import pallas as pl
from jax.experimental.pallas import tpu as pltpu
from jax.sharding import PartitionSpec as P

epsilon = 1e-06
LANES = 128
STAGGER_NS = 28000


VMEM = pl.BlockSpec(memory_space=pltpu.VMEM)
HBM = pl.BlockSpec(memory_space=pltpu.HBM)


def in_vmem(arrays):
    return [pltpu.with_memory_space_constraint(a, pltpu.VMEM) for a in arrays]


def in_hbm(arrays):
    return [pltpu.with_memory_space_constraint(a, pltpu.HBM) for a in arrays]


def pack_kernel(
    capacity,
    tokens_hbm,
    gain_hbm,
    ids_hbm,
    normed_hbm,
    out_hbm,
    pos_hbm,
    tokens,
    gain_ref,
    ids_ref,
    pos_ref,
    normed,
    packed,
    tiles,
    pos_smem,
    sems,
):
    rows, width = tokens.shape
    per_row = width // LANES
    top_count = ids_ref.shape[0]
    experts = packed.shape[0] // per_row // capacity
    ids_load = pltpu.make_async_copy(ids_hbm, ids_ref, sems.at[4])
    gain_load = pltpu.make_async_copy(gain_hbm, gain_ref, sems.at[5])
    load = pltpu.make_async_copy(tokens_hbm, tokens, sems.at[0])
    for copy in (ids_load, gain_load, load):
        copy.start()
    ids_load.wait()
    ids = ids_ref[...]
    expert_iota = lax.broadcasted_iota(jnp.int32, (experts, rows), 0)
    named = [jnp.where(expert_iota == ids[j : j + 1, :], 1.0, 0.0) for j in range(top_count)]
    total = sum(named[1:], named[0]).astype(jnp.bfloat16)
    earlier = jnp.where(
        lax.broadcasted_iota(jnp.int32, (rows, rows), 0) < lax.broadcasted_iota(jnp.int32, (rows, rows), 1), 1.0, 0.0
    ).astype(jnp.bfloat16)
    before = jnp.dot(total, earlier, preferred_element_type=jnp.float32)
    for j in range(top_count):
        slot = jnp.sum(before * named[j], axis=0, keepdims=True).astype(jnp.int32)
        pos_ref[j : j + 1, :] = ids[j : j + 1, :] * capacity + slot
    scalars = pltpu.make_async_copy(pos_ref, pos_smem, sems.at[1])
    scalars.start()
    pos_keep = pltpu.make_async_copy(pos_ref, pos_hbm, sems.at[6])
    pos_keep.start()
    gain_load.wait()
    gain = gain_ref[...]
    step = 16
    load.wait()

    def norm_rows(i, carry):
        first = pl.multiple_of(i * step, step)
        values = tokens[pl.ds(first, step), :].astype(jnp.float32)
        factor = lax.rsqrt(jnp.mean(values * values, axis=1, keepdims=True) + epsilon)
        rounded = (values * factor * gain).astype(jnp.bfloat16)
        normed[pl.ds(first, step), :] = rounded
        wide = rounded.astype(jnp.float32)
        for k in range(per_row):
            tiles[pl.ds(first * per_row + k, step, stride=per_row), :] = wide[:, k * LANES : (k + 1) * LANES]
        return carry

    lax.fori_loop(0, rows // step, norm_rows, 0, unroll=8)
    keep = pltpu.make_async_copy(normed, normed_hbm, sems.at[2])
    keep.start()
    scalars.wait()

    unroll = 16

    def place(i, carry):
        for u in range(unroll):
            row = i * unroll + u
            tile = tiles[pl.ds(pl.multiple_of(row * per_row, per_row), per_row), :].astype(jnp.bfloat16)
            for j in range(top_count):
                at = pl.multiple_of(pos_smem[j, row] * per_row, per_row)
                packed[pl.ds(at, per_row), :] = tile
        return carry

    lax.fori_loop(0, rows // unroll, place, 0)
    send = pltpu.make_async_copy(packed, out_hbm, sems.at[3])
    send.start()
    pos_keep.wait()
    keep.wait()
    send.wait()

    @pl.when(lax.axis_index("tp") == 0)
    def _():
        pl.delay(STAGGER_NS)


def pack(tokens, norm_gain, ids, experts, capacity):
    rows, width = tokens.shape
    per_row = width // LANES
    top_count = ids.shape[0]
    slots = experts * capacity * per_row
    return pl.pallas_call(
        functools.partial(pack_kernel, capacity),
        out_shape=(
            pltpu.HBM((rows, width), jnp.bfloat16),
            pltpu.HBM((slots, LANES), jnp.bfloat16),
            pltpu.HBM((top_count, rows), jnp.int32),
        ),
        in_specs=[HBM] * 3,
        out_specs=(HBM,) * 3,
        scratch_shapes=[
            pltpu.VMEM((rows, width), jnp.bfloat16),
            pltpu.VMEM((1, width), jnp.float32),
            pltpu.VMEM((top_count, rows), jnp.int32),
            pltpu.VMEM((top_count, rows), jnp.int32),
            pltpu.VMEM((rows, width), jnp.bfloat16),
            pltpu.VMEM((slots, LANES), jnp.bfloat16),
            pltpu.VMEM((rows * per_row, LANES), jnp.float32),
            pltpu.SMEM((top_count, rows), jnp.int32),
            pltpu.SemaphoreType.DMA((7,)),
        ],
        compiler_params=pltpu.CompilerParams(vmem_limit_bytes=20 << 20),
        cost_estimate=pl.CostEstimate(flops=2 * experts * rows * rows, bytes_accessed=6 << 20, transcendentals=rows),
        name="pack_rows",
    )(*in_hbm([tokens, norm_gain.reshape(1, width), ids]))


def gated_sum(rows, gates, ups, downs):
    total = None
    for gate, up, down in zip(gates, ups, downs):
        gate_value = jnp.dot(rows, gate[...], preferred_element_type=jnp.float32)
        up_value = jnp.dot(rows, up[...], preferred_element_type=jnp.float32)
        hidden = (gate_value / (1.0 + jnp.exp(-gate_value)) * up_value).astype(jnp.bfloat16)
        part = jnp.dot(hidden, down[...], preferred_element_type=jnp.float32)
        part = part.astype(jnp.bfloat16).astype(jnp.float32)
        total = part if total is None else total + part
    return total


def expert_kernel(blocks, rows_ref, *refs):
    weights_hbm, out_hbm, weights = refs[:6], refs[6], refs[7:13]
    tiles, rows, results, weight_sems, out_sems = refs[13:]
    total_rows, width = rows.shape
    per_row = width // LANES
    block = total_rows // blocks
    loads = [pltpu.make_async_copy(h, w, weight_sems.at[i]) for i, (h, w) in enumerate(zip(weights_hbm, weights))]
    for load in loads:
        load.start()

    def tile_range(i):
        return pl.ds(pl.multiple_of(i * block * per_row, block * per_row), block * per_row)

    def row_range(i):
        return pl.ds(pl.multiple_of(i * block, block), block)

    def untile(i, carry):
        tiles[...] = rows_ref[tile_range(i), :].astype(jnp.float32)
        for k in range(per_row):
            piece = tiles[pl.ds(k, block, stride=per_row), :]
            rows[row_range(i), k * LANES : (k + 1) * LANES] = piece.astype(jnp.bfloat16)
        return carry

    lax.fori_loop(0, blocks, untile, 0)
    for load in loads:
        load.wait()

    def store(i):
        return pltpu.make_async_copy(results.at[tile_range(i)], out_hbm.at[tile_range(i)], out_sems.at[i])

    def one_block(i, carry):
        total = gated_sum(rows[row_range(i), :], (weights[0], weights[3]), (weights[1], weights[4]), (weights[2], weights[5]))
        for k in range(per_row):
            tiles[pl.ds(k, block, stride=per_row), :] = total[:, k * LANES : (k + 1) * LANES]
        results[tile_range(i), :] = tiles[...].astype(jnp.bfloat16)
        store(i).start()
        return carry

    lax.fori_loop(0, blocks, one_block, 0)
    for i in range(blocks):
        store(i).wait()


def shared_kernel(rows_hbm, *refs):
    sources, out_hbm, held, out, sems = (rows_hbm, *refs[:6]), refs[6], refs[7:14], refs[14], refs[15]
    loads = [pltpu.make_async_copy(h, w, sems.at[i]) for i, (h, w) in enumerate(zip(sources, held))]
    for load in loads:
        load.start()
    for load in loads:
        load.wait()
    out[...] = gated_sum(held[0][...], (held[1], held[4]), (held[2], held[5]), (held[3], held[6]))
    store = pltpu.make_async_copy(out, out_hbm, sems.at[7])
    store.start()
    store.wait()


def ffn_cost(rows, weights):
    flops = 2 * rows * sum(w.shape[0] * w.shape[1] for w in weights)
    return pl.CostEstimate(flops=flops, bytes_accessed=12 << 20, transcendentals=rows * 512)


def expert_ffn(received, weights):
    width = weights[0].shape[0]
    per_row = width // LANES
    rows = received.shape[0] // per_row
    blocks = 2
    return pl.pallas_call(
        functools.partial(expert_kernel, blocks),
        out_shape=pltpu.HBM(received.shape, jnp.bfloat16),
        in_specs=[VMEM] + [HBM] * 6,
        out_specs=HBM,
        scratch_shapes=[pltpu.VMEM(w.shape, w.dtype) for w in weights]
        + [
            pltpu.VMEM((rows // blocks * per_row, LANES), jnp.float32),
            pltpu.VMEM((rows, width), jnp.bfloat16),
            pltpu.VMEM(received.shape, jnp.bfloat16),
            pltpu.SemaphoreType.DMA((6,)),
            pltpu.SemaphoreType.DMA((blocks,)),
        ],
        compiler_params=pltpu.CompilerParams(vmem_limit_bytes=40 << 20),
        cost_estimate=ffn_cost(rows, weights),
        name="expert_ffn",
    )(*in_vmem([received]), *in_hbm(weights))


def shared_ffn(normed, weights):
    rows, width = normed.shape
    return pl.pallas_call(
        shared_kernel,
        out_shape=pltpu.HBM((rows, width), jnp.float32),
        in_specs=[HBM] * 7,
        out_specs=HBM,
        scratch_shapes=[pltpu.VMEM(a.shape, a.dtype) for a in [normed] + weights]
        + [pltpu.VMEM((rows, width), jnp.float32), pltpu.SemaphoreType.DMA((8,))],
        compiler_params=pltpu.CompilerParams(vmem_limit_bytes=30 << 20),
        cost_estimate=ffn_cost(rows, weights),
        name="shared_ffn",
    )(*in_hbm([normed] + weights))


def combine_kernel(pos_hbm, weight_hbm, returned_ref, shared_hbm, out_hbm, pos_ref, weight_ref, shared, tiles, out, load_sems, out_sems):
    rows, width = out.shape
    per_row = width // LANES
    top_count = pos_ref.shape[0]
    scalars = [
        pltpu.make_async_copy(pos_hbm, pos_ref, load_sems.at[0]),
        pltpu.make_async_copy(weight_hbm, weight_ref, load_sems.at[1]),
    ]
    load = pltpu.make_async_copy(shared_hbm, shared, load_sems.at[2])
    for copy in scalars + [load]:
        copy.start()
    unroll = 16
    parts = out_sems.shape[0]
    part = rows // parts
    step = 16

    def mix(i, carry):
        for u in range(unroll):
            row = i * unroll + u
            total = None
            for j in range(top_count):
                at = pl.multiple_of(pos_ref[j, row] * per_row, per_row)
                term = returned_ref[pl.ds(at, per_row), :].astype(jnp.float32) * weight_ref[j, row]
                total = term if total is None else total + term
            tiles[pl.ds(pl.multiple_of(row * per_row, per_row), per_row), :] = total
        return carry

    def finish(i, carry):
        first = pl.multiple_of(i * step, step)
        for k in range(per_row):
            cols = slice(k * LANES, (k + 1) * LANES)
            routed = tiles[pl.ds(first * per_row + k, step, stride=per_row), :]
            out[pl.ds(first, step), cols] = (routed + shared[pl.ds(first, step), cols]).astype(jnp.bfloat16)
        return carry

    stores = []
    for copy in scalars:
        copy.wait()
    for p in range(parts):
        lax.fori_loop(p * part // unroll, (p + 1) * part // unroll, mix, 0)
        if p == 0:
            load.wait()
        lax.fori_loop(p * part // step, (p + 1) * part // step, finish, 0, unroll=2)
        at = pl.ds(p * part, part)
        stores.append(pltpu.make_async_copy(out.at[at], out_hbm.at[at], out_sems.at[p]))
        stores[-1].start()
    for store in stores:
        store.wait()


def combine(pos, route_weights, returned, shared_out):
    rows, width = shared_out.shape
    per_row = width // LANES
    return pl.pallas_call(
        combine_kernel,
        out_shape=pltpu.HBM((rows, width), jnp.bfloat16),
        in_specs=[HBM, HBM, VMEM, HBM],
        out_specs=HBM,
        scratch_shapes=[
            pltpu.SMEM(pos.shape, pos.dtype),
            pltpu.SMEM(route_weights.shape, route_weights.dtype),
            pltpu.VMEM((rows, width), jnp.float32),
            pltpu.VMEM((rows * per_row, LANES), jnp.float32),
            pltpu.VMEM((rows, width), jnp.bfloat16),
            pltpu.SemaphoreType.DMA((3,)),
            pltpu.SemaphoreType.DMA((2,)),
        ],
        compiler_params=pltpu.CompilerParams(vmem_limit_bytes=20 << 20),
        cost_estimate=pl.CostEstimate(flops=4 * rows * width, bytes_accessed=6 << 20, transcendentals=0),
        name="combine_rows",
    )(*in_hbm([pos, route_weights]), *in_vmem([returned]), *in_hbm([shared_out]))


def swapped(own):
    pairs = [(i, lax.axis_size("tp") - 1 - i) for i in range(lax.axis_size("tp"))]
    return [lax.ppermute(w, "tp", pairs) for w in own]


def body(
    tokens,
    norm_gain,
    expert_ids,
    route_weights,
    expert_gate,
    expert_up,
    expert_down,
    shared_gate,
    shared_up,
    shared_down,
):
    tok_rows, width = tokens.shape
    top_count = expert_ids.shape[1]
    ep_size = lax.axis_size("ep")
    experts = expert_gate.shape[0] * ep_size
    capacity = 3 * tok_rows * top_count // (2 * experts)
    per_row = width // LANES
    normed, outgoing, pos = pack(tokens, norm_gain, expert_ids.T, experts, capacity)

    def exchange(rows):
        split = rows.reshape(ep_size, capacity * per_row, LANES)
        moved = lax.all_to_all(split, "ep", split_axis=0, concat_axis=0, tiled=True)
        return moved.reshape(rows.shape)

    received = exchange(outgoing)
    expert_own = [expert_gate[0], expert_up[0], expert_down[0]]
    shared_own = [shared_gate, shared_up, shared_down]
    shared_out = shared_ffn(normed, shared_own + swapped(shared_own))
    results = expert_ffn(received, expert_own + swapped(expert_own))
    returned = exchange(results)
    return combine(pos, route_weights.T, returned, shared_out)


def solution(mesh):
    placed = (
        P(("ep", "tp"), None),
        P(),
        P(("ep", "tp"), None),
        P(("ep", "tp"), None),
        P("ep", None, "tp"),
        P("ep", None, "tp"),
        P("ep", "tp", None),
        P(None, "tp"),
        P(None, "tp"),
        P("tp", None),
    )
    return jax.shard_map(
        body, mesh=mesh, in_specs=placed, out_specs=P(("ep", "tp"), None), check_vma=False
    )
```

```python
import functools

import jax
import jax.numpy as jnp
from jax import lax
from jax.experimental import pallas as pl
from jax.experimental.pallas import tpu as pltpu
from jax.sharding import PartitionSpec as P

epsilon = 1e-06
LANES = 128
STAGGER_NS = 28000


VMEM = pl.BlockSpec(memory_space=pltpu.VMEM)
HBM = pl.BlockSpec(memory_space=pltpu.HBM)


def in_vmem(arrays):
    return [pltpu.with_memory_space_constraint(a, pltpu.VMEM) for a in arrays]


def in_hbm(arrays):
    return [pltpu.with_memory_space_constraint(a, pltpu.HBM) for a in arrays]


def pack_kernel(
    capacity,
    tokens_hbm,
    gain_hbm,
    ids_hbm,
    out_hbm,
    pos_hbm,
    tokens,
    gain_ref,
    ids_ref,
    pos_ref,
    packed,
    tiles,
    pos_smem,
    sems,
):
    rows, width = tokens.shape
    per_row = width // LANES
    top_count = ids_ref.shape[0]
    experts = packed.shape[0] // per_row // capacity
    ids_load = pltpu.make_async_copy(ids_hbm, ids_ref, sems.at[4])
    gain_load = pltpu.make_async_copy(gain_hbm, gain_ref, sems.at[5])
    load = pltpu.make_async_copy(tokens_hbm, tokens, sems.at[0])
    for copy in (ids_load, gain_load, load):
        copy.start()
    ids_load.wait()
    ids = ids_ref[...]
    expert_iota = lax.broadcasted_iota(jnp.int32, (experts, rows), 0)
    named = [jnp.where(expert_iota == ids[j : j + 1, :], 1.0, 0.0) for j in range(top_count)]
    total = sum(named[1:], named[0]).astype(jnp.bfloat16)
    earlier = jnp.where(
        lax.broadcasted_iota(jnp.int32, (rows, rows), 0) < lax.broadcasted_iota(jnp.int32, (rows, rows), 1), 1.0, 0.0
    ).astype(jnp.bfloat16)
    before = jnp.dot(total, earlier, preferred_element_type=jnp.float32)
    for j in range(top_count):
        slot = jnp.sum(before * named[j], axis=0, keepdims=True).astype(jnp.int32)
        pos_ref[j : j + 1, :] = ids[j : j + 1, :] * capacity + slot
    scalars = pltpu.make_async_copy(pos_ref, pos_smem, sems.at[1])
    scalars.start()
    pos_keep = pltpu.make_async_copy(pos_ref, pos_hbm, sems.at[2])
    pos_keep.start()
    gain_load.wait()
    gain = gain_ref[...]
    step = 16
    load.wait()

    def norm_rows(i, carry):
        first = pl.multiple_of(i * step, step)
        values = tokens[pl.ds(first, step), :].astype(jnp.float32)
        factor = lax.rsqrt(jnp.mean(values * values, axis=1, keepdims=True) + epsilon)
        rounded = (values * factor * gain).astype(jnp.bfloat16)
        wide = rounded.astype(jnp.float32)
        for k in range(per_row):
            tiles[pl.ds(first * per_row + k, step, stride=per_row), :] = wide[:, k * LANES : (k + 1) * LANES]
        return carry

    lax.fori_loop(0, rows // step, norm_rows, 0, unroll=8)
    scalars.wait()

    unroll = 32

    def place(i, carry):
        for u in range(unroll):
            row = i * unroll + u
            tile = tiles[pl.ds(pl.multiple_of(row * per_row, per_row), per_row), :].astype(jnp.bfloat16)
            for j in range(top_count):
                at = pl.multiple_of(pos_smem[j, row] * per_row, per_row)
                packed[pl.ds(at, per_row), :] = tile
        return carry

    lax.fori_loop(0, rows // unroll, place, 0)
    send = pltpu.make_async_copy(packed, out_hbm, sems.at[3])
    send.start()
    pos_keep.wait()
    send.wait()

    @pl.when(lax.axis_index("tp") == 0)
    def _():
        pl.delay(STAGGER_NS)


def pack(tokens, norm_gain, ids, experts, capacity):
    rows, width = tokens.shape
    per_row = width // LANES
    top_count = ids.shape[0]
    slots = experts * capacity * per_row
    return pl.pallas_call(
        functools.partial(pack_kernel, capacity),
        out_shape=(
            pltpu.HBM((slots, LANES), jnp.bfloat16),
            pltpu.HBM((top_count, rows), jnp.int32),
        ),
        in_specs=[HBM] * 3,
        out_specs=(HBM,) * 2,
        scratch_shapes=[
            pltpu.VMEM((rows, width), jnp.bfloat16),
            pltpu.VMEM((1, width), jnp.float32),
            pltpu.VMEM((top_count, rows), jnp.int32),
            pltpu.VMEM((top_count, rows), jnp.int32),
            pltpu.VMEM((slots, LANES), jnp.bfloat16),
            pltpu.VMEM((rows * per_row, LANES), jnp.float32),
            pltpu.SMEM((top_count, rows), jnp.int32),
            pltpu.SemaphoreType.DMA((6,)),
        ],
        compiler_params=pltpu.CompilerParams(vmem_limit_bytes=20 << 20),
        cost_estimate=pl.CostEstimate(flops=2 * experts * rows * rows, bytes_accessed=6 << 20, transcendentals=rows),
        name="pack_rows",
    )(*in_hbm([tokens, norm_gain.reshape(1, width), ids]))


def gated_sum(rows, gates, ups, downs):
    total = None
    for gate, up, down in zip(gates, ups, downs):
        gate_value = jnp.dot(rows, gate[...], preferred_element_type=jnp.float32)
        up_value = jnp.dot(rows, up[...], preferred_element_type=jnp.float32)
        hidden = (gate_value / (1.0 + jnp.exp(-gate_value)) * up_value).astype(jnp.bfloat16)
        part = jnp.dot(hidden, down[...], preferred_element_type=jnp.float32)
        part = part.astype(jnp.bfloat16).astype(jnp.float32)
        total = part if total is None else total + part
    return total


def expert_kernel(blocks, rows_ref, *refs):
    weights_hbm, out_hbm, weights = refs[:6], refs[6], refs[7:13]
    tiles, rows, results, weight_sems, out_sems = refs[13:]
    total_rows, width = rows.shape
    per_row = width // LANES
    block = total_rows // blocks
    loads = [pltpu.make_async_copy(h, w, weight_sems.at[i]) for i, (h, w) in enumerate(zip(weights_hbm, weights))]
    for load in loads:
        load.start()

    def tile_range(i):
        return pl.ds(pl.multiple_of(i * block * per_row, block * per_row), block * per_row)

    def row_range(i):
        return pl.ds(pl.multiple_of(i * block, block), block)

    def untile(i, carry):
        tiles[...] = rows_ref[tile_range(i), :].astype(jnp.float32)
        for k in range(per_row):
            piece = tiles[pl.ds(k, block, stride=per_row), :]
            rows[row_range(i), k * LANES : (k + 1) * LANES] = piece.astype(jnp.bfloat16)
        return carry

    lax.fori_loop(0, blocks, untile, 0)
    for load in loads:
        load.wait()

    def store(i):
        return pltpu.make_async_copy(results.at[tile_range(i)], out_hbm.at[tile_range(i)], out_sems.at[i])

    def one_block(i, carry):
        total = gated_sum(rows[row_range(i), :], (weights[0], weights[3]), (weights[1], weights[4]), (weights[2], weights[5]))
        for k in range(per_row):
            tiles[pl.ds(k, block, stride=per_row), :] = total[:, k * LANES : (k + 1) * LANES]
        results[tile_range(i), :] = tiles[...].astype(jnp.bfloat16)
        store(i).start()
        return carry

    lax.fori_loop(0, blocks, one_block, 0)
    for i in range(blocks):
        store(i).wait()


def shared_kernel(rows_hbm, *refs):
    sources, out_hbm, held, out, sems = (rows_hbm, *refs[:7]), refs[7], refs[8:16], refs[16], refs[17]
    loads = [pltpu.make_async_copy(h, w, sems.at[i]) for i, (h, w) in enumerate(zip(sources, held))]
    for load in loads:
        load.start()
    for load in loads:
        load.wait()
    values = held[0][...].astype(jnp.float32)
    factor = lax.rsqrt(jnp.mean(values * values, axis=1, keepdims=True) + epsilon)
    normed = (values * factor * held[7][...]).astype(jnp.bfloat16)
    out[...] = gated_sum(normed, (held[1], held[4]), (held[2], held[5]), (held[3], held[6]))
    store = pltpu.make_async_copy(out, out_hbm, sems.at[8])
    store.start()
    store.wait()


def ffn_cost(rows, weights):
    flops = 2 * rows * sum(w.shape[0] * w.shape[1] for w in weights)
    return pl.CostEstimate(flops=flops, bytes_accessed=12 << 20, transcendentals=rows * 512)


def expert_ffn(received, weights):
    width = weights[0].shape[0]
    per_row = width // LANES
    rows = received.shape[0] // per_row
    blocks = 2
    return pl.pallas_call(
        functools.partial(expert_kernel, blocks),
        out_shape=pltpu.HBM(received.shape, jnp.bfloat16),
        in_specs=[VMEM] + [HBM] * 6,
        out_specs=HBM,
        scratch_shapes=[pltpu.VMEM(w.shape, w.dtype) for w in weights]
        + [
            pltpu.VMEM((rows // blocks * per_row, LANES), jnp.float32),
            pltpu.VMEM((rows, width), jnp.bfloat16),
            pltpu.VMEM(received.shape, jnp.bfloat16),
            pltpu.SemaphoreType.DMA((6,)),
            pltpu.SemaphoreType.DMA((blocks,)),
        ],
        compiler_params=pltpu.CompilerParams(vmem_limit_bytes=40 << 20),
        cost_estimate=ffn_cost(rows, weights),
        name="expert_ffn",
    )(*in_vmem([received]), *in_hbm(weights))


def shared_ffn(tokens, weights, norm_gain):
    rows, width = tokens.shape
    operands = [tokens] + weights + [norm_gain.reshape(1, width)]
    return pl.pallas_call(
        shared_kernel,
        out_shape=pltpu.HBM((rows, width), jnp.float32),
        in_specs=[HBM] * 8,
        out_specs=HBM,
        scratch_shapes=[pltpu.VMEM(a.shape, a.dtype) for a in operands]
        + [pltpu.VMEM((rows, width), jnp.float32), pltpu.SemaphoreType.DMA((9,))],
        compiler_params=pltpu.CompilerParams(vmem_limit_bytes=30 << 20),
        cost_estimate=ffn_cost(rows, weights),
        name="shared_ffn",
    )(*in_hbm(operands))


def combine_kernel(pos_hbm, weight_hbm, returned_ref, shared_hbm, out_hbm, pos_ref, weight_ref, shared, tiles, out, load_sems, out_sems):
    rows, width = out.shape
    per_row = width // LANES
    top_count = pos_ref.shape[0]
    scalars = [
        pltpu.make_async_copy(pos_hbm, pos_ref, load_sems.at[0]),
        pltpu.make_async_copy(weight_hbm, weight_ref, load_sems.at[1]),
    ]
    load = pltpu.make_async_copy(shared_hbm, shared, load_sems.at[2])
    for copy in scalars + [load]:
        copy.start()
    unroll = 16
    parts = out_sems.shape[0]
    part = rows // parts
    step = 16

    def mix(i, carry):
        for u in range(unroll):
            row = i * unroll + u
            total = None
            for j in range(top_count):
                at = pl.multiple_of(pos_ref[j, row] * per_row, per_row)
                term = returned_ref[pl.ds(at, per_row), :].astype(jnp.float32) * weight_ref[j, row]
                total = term if total is None else total + term
            tiles[pl.ds(pl.multiple_of(row * per_row, per_row), per_row), :] = total
        return carry

    def finish(i, carry):
        first = pl.multiple_of(i * step, step)
        for k in range(per_row):
            cols = slice(k * LANES, (k + 1) * LANES)
            routed = tiles[pl.ds(first * per_row + k, step, stride=per_row), :]
            out[pl.ds(first, step), cols] = (routed + shared[pl.ds(first, step), cols]).astype(jnp.bfloat16)
        return carry

    stores = []
    for copy in scalars:
        copy.wait()
    for p in range(parts):
        lax.fori_loop(p * part // unroll, (p + 1) * part // unroll, mix, 0)
        if p == 0:
            load.wait()
        lax.fori_loop(p * part // step, (p + 1) * part // step, finish, 0, unroll=2)
        at = pl.ds(p * part, part)
        stores.append(pltpu.make_async_copy(out.at[at], out_hbm.at[at], out_sems.at[p]))
        stores[-1].start()
    for store in stores:
        store.wait()


def combine(pos, route_weights, returned, shared_out):
    rows, width = shared_out.shape
    per_row = width // LANES
    return pl.pallas_call(
        combine_kernel,
        out_shape=pltpu.HBM((rows, width), jnp.bfloat16),
        in_specs=[HBM, HBM, VMEM, HBM],
        out_specs=HBM,
        scratch_shapes=[
            pltpu.SMEM(pos.shape, pos.dtype),
            pltpu.SMEM(route_weights.shape, route_weights.dtype),
            pltpu.VMEM((rows, width), jnp.float32),
            pltpu.VMEM((rows * per_row, LANES), jnp.float32),
            pltpu.VMEM((rows, width), jnp.bfloat16),
            pltpu.SemaphoreType.DMA((3,)),
            pltpu.SemaphoreType.DMA((2,)),
        ],
        compiler_params=pltpu.CompilerParams(vmem_limit_bytes=20 << 20),
        cost_estimate=pl.CostEstimate(flops=4 * rows * width, bytes_accessed=6 << 20, transcendentals=0),
        name="combine_rows",
    )(*in_hbm([pos, route_weights]), *in_vmem([returned]), *in_hbm([shared_out]))


def swapped(own):
    pairs = [(i, lax.axis_size("tp") - 1 - i) for i in range(lax.axis_size("tp"))]
    return [lax.ppermute(w, "tp", pairs) for w in own]


def body(
    tokens,
    norm_gain,
    expert_ids,
    route_weights,
    expert_gate,
    expert_up,
    expert_down,
    shared_gate,
    shared_up,
    shared_down,
):
    tok_rows, width = tokens.shape
    top_count = expert_ids.shape[1]
    ep_size = lax.axis_size("ep")
    experts = expert_gate.shape[0] * ep_size
    capacity = 3 * tok_rows * top_count // (2 * experts)
    per_row = width // LANES
    outgoing, pos = pack(tokens, norm_gain, expert_ids.T, experts, capacity)

    def exchange(rows):
        split = rows.reshape(ep_size, capacity * per_row, LANES)
        moved = lax.all_to_all(split, "ep", split_axis=0, concat_axis=0, tiled=True)
        return moved.reshape(rows.shape)

    received = exchange(outgoing)
    expert_own = [expert_gate[0], expert_up[0], expert_down[0]]
    shared_own = [shared_gate, shared_up, shared_down]
    shared_out = shared_ffn(tokens, shared_own + swapped(shared_own), norm_gain)
    results = expert_ffn(received, expert_own + swapped(expert_own))
    returned = exchange(results)
    return combine(pos, route_weights.T, returned, shared_out)


def solution(mesh):
    placed = (
        P(("ep", "tp"), None),
        P(),
        P(("ep", "tp"), None),
        P(("ep", "tp"), None),
        P("ep", None, "tp"),
        P("ep", None, "tp"),
        P("ep", "tp", None),
        P(None, "tp"),
        P(None, "tp"),
        P("tp", None),
    )
    return jax.shard_map(
        body, mesh=mesh, in_specs=placed, out_specs=P(("ep", "tp"), None), check_vma=False
    )
```
